32 devices in a mesh: sp: 4 (over y, x), tp: 8 (over z, core).
Axes of the slice: x: 2, y: 2, z: 4, core: 2. Of those that a mesh axis runs over, the one named last changes fastest.
Arguments:
- queries: bfloat16 [1536, 2048], P('sp', 'tp'), may hold values from -6 to 6
- keys: bfloat16 [1536, 2048], P('sp', 'tp'), may hold values from -6 to 6
- values: bfloat16 [1536, 2048], P('sp', 'tp'), may hold values from -6 to 6
- key_bias: bfloat16 [1536, 32], P('sp', 'tp'), may hold values from -16 to 0
- head_gain: float32 [32, 64], P('tp'), may hold values from 0.1 to 1.9
- out_weight: bfloat16 [2048, 2048], P('tp'), may hold values from -0.125 to 0.125
- residual: bfloat16 [1536, 2048], P(('sp', 'tp')), may hold values from -6 to 6
- norm_gain: float32 [2048], replicated, may hold values from 0.1 to 1.9
- gate_proj: bfloat16 [4, 2048, 7168], P('sp', None, 'tp'), may hold values from -0.125 to 0.125
- up_proj: bfloat16 [4, 2048, 7168], P('sp', None, 'tp'), may hold values from -0.125 to 0.125
- down_proj: bfloat16 [4, 7168, 2048], P('sp', 'tp'), may hold values from -0.0625 to 0.0625
- expert_choice: int32 [1536, 2], P(('sp', 'tp')), may hold values from 0 to 3, all different within a row; in each aligned block of 48 rows (0 to 47, 48 to 95, ...) at most 48 rows name the same one
- expert_weights: float32 [1536, 2], P(('sp', 'tp')), may hold values from 0.2 to 1
Outputs:
- layer_out: bfloat16 [1536, 2048], P(('sp', 'tp'))
The draws below stay inside these ranges and needn't reach their ends.
Inputs may be any that keep to these rules, and one draw needn't show every extreme that they name: `expert_choice`: in each aligned block of 48 rows (the rows of one device), no expert is named more than 48 times; the two experts of a row differ.
All inputs are finite; a program needn't handle non-finite values.
Results may differ from the reference program's by a relative error of at most 0.019.
Values may be sent and summed in bfloat16 or wider, within the bound.
A program may use at most 128 MiB of HBM per device.

```python
import math
import jax
import jax.numpy as jnp
import numpy as np
from jax import lax

D = 2048
HEADS = 32
HEAD_DIM = 64
FFE = 7168
TOK_DEV = 384
TOKENS = 1536
EXPERTS = 4
ROWS_DEV = 48
CAP = 48
N_TP = 8


def draw_key_bias(key, part):
    streams = jax.random.split(jax.random.fold_in(key, 11), 7)
    chance = 0.5
    slow_heads = jax.random.uniform(streams[0], (HEADS,)) < chance
    fast_base = jax.random.uniform(streams[1], (HEADS,), minval=-5.0, maxval=-3.8)
    slow_base = -jnp.log(jnp.float32(TOKENS)) - 0.5 + jax.random.uniform(streams[2], (HEADS,), minval=-0.5, maxval=0.5)
    blocks = TOKENS // TOK_DEV
    device_factor = jax.random.uniform(streams[3], (blocks, 1, HEADS), minval=-0.7, maxval=0.7)
    device_factor = jnp.broadcast_to(device_factor, (blocks, TOK_DEV, HEADS)).reshape(TOKENS, HEADS)
    jitter = 0.3 * jax.random.normal(streams[4], (TOKENS, HEADS))
    base = jnp.where(slow_heads[None, :], slow_base[None, :], fast_base[None, :]) + device_factor + jitter
    spots = jax.random.randint(streams[5], (2,), 0, TOKENS)
    levels = jax.random.uniform(streams[6], (2, HEADS), minval=-1.4, maxval=0.0)
    position = jnp.arange(TOKENS)
    first_hit = (position == spots[0])[:, None] & slow_heads[None, :]
    second_hit = (position == spots[1])[:, None] & slow_heads[None, :]
    base = jnp.where(first_hit, levels[0][None, :], base)
    base = jnp.where(second_hit, levels[1][None, :], base)
    return jnp.clip(base, -16.0, 0.0).astype(jnp.bfloat16)


def block_levels(stream_key, extent, pieces, smallest, top_value):
    factor_of, own = 1.0, jax.random.fold_in(stream_key, 6)
    for dim, blocks in pieces:
        heights = jnp.exp(jax.random.uniform(jax.random.fold_in(own, dim), (blocks,), jnp.float32, smallest / len(pieces), top_value / len(pieces)))
        factor_of = factor_of * jnp.repeat(heights, extent[dim] // blocks).reshape([-1 if axis == dim else 1 for axis in range(len(extent))])
    return factor_of


def assign_block(key, own, number, rows, count, top, bound, skew):
    sequence = jax.random.permutation(key, count)
    heavy_load, ordinary = shares(count, rows * top, bound, skew, True), shares(count, rows * top, bound, skew, False)
    places = jnp.arange(count)

    def named(tallies, rotation):
        used = int((tallies > 0).sum())
        fixed = max(1, used // 4)
        shifted = fixed + (places - fixed + rotation * (used - fixed)) % max(1, count - fixed)
        return jnp.zeros((count,), jnp.int32).at[sequence[jnp.where(places < fixed, places, shifted)]].set(jnp.asarray(tallies, jnp.int32))

    tallies = jnp.where(number % 4 == 0, named(heavy_load, number // 4), named(ordinary, number - number // 4 - 1))
    mixed = jax.random.permutation(jax.random.fold_in(own, 3), count)
    giver, taker = mixed[0:count // 2 * 2:2], mixed[1:count // 2 * 2:2]
    margin = jnp.minimum(tallies[giver] - 1, bound - tallies[taker]) // 2
    margin = jnp.where((giver == sequence[0]) | (taker == sequence[0]) | (tallies[taker] == 0), 0, jnp.maximum(margin, 0))
    shifted = jax.random.randint(jax.random.fold_in(own, 4), (count // 2,), 0, 1 << 20) % (margin + 1)
    tallies = tallies.at[giver].add(-shifted).at[taker].add(shifted)
    items = jnp.searchsorted(jnp.cumsum(tallies), jnp.arange(rows * top), side="right").astype(jnp.int32)
    table = items.reshape(top, rows).T
    table = table[jax.random.permutation(jax.random.fold_in(own, 1), rows)]
    rotation = jax.random.randint(jax.random.fold_in(own, 2), (rows, 1), 0, top)
    return jnp.take_along_axis(table, (jnp.arange(top)[None, :] + rotation) % top, axis=1)


def shares(count, total, limit, slope, full):
    weights = [(1 << 20) // math.isqrt(standing ** slope) + 1 for standing in range(1, count + 1)]
    largest = limit if full else min(limit, max(-(-total // count), total * weights[0] // sum(weights)))
    least = 1 if total - largest >= count - 1 else 0
    counts, spare = [largest] + [least] * (count - 1), total - largest - least * (count - 1)
    while spare > 0:
        movable = [i for i in range(1, count) if counts[i] < largest] or [i for i in range(1, count) if counts[i] < limit]
        whole, remaining = sum([weights[i] for i in movable]), spare
        for i in movable:
            addition = min(limit - counts[i], max(1, remaining * weights[i] // whole), spare)
            counts[i] = counts[i] + addition
            spare = spare - addition
    return np.array(counts)


def scatter_about(key, shape, spread, reach, shards=(), held_as=jnp.bfloat16):
    gain = block_levels(key, shape, shards, -0.22, 0.18) if shards else 1.0
    values = jax.random.normal(key, shape, jnp.float32) * spread * gain
    return jnp.minimum(jnp.maximum(values, -reach), reach).astype(held_as)


def setup_inputs(seed: int = 0) -> dict:
    key_of = jax.random.split(jax.random.key(seed), 14)
    queries = scatter_about(key_of[0], (TOKENS, HEADS * HEAD_DIM), 1.0, 6.0, ((0, 4), (1, 8)))
    keys = scatter_about(key_of[1], (TOKENS, HEADS * HEAD_DIM), 1.0, 6.0, ((0, 4), (1, 8)))
    values = scatter_about(key_of[2], (TOKENS, HEADS * HEAD_DIM), 1.0, 6.0, ((0, 4), (1, 8)))
    key_bias = draw_key_bias(jax.random.fold_in(key_of[13], 71), 0)
    head_gain = jnp.clip(1.0 + 0.18 * jax.random.normal(key_of[4], (HEADS, HEAD_DIM), jnp.float32), 0.1, 1.9)
    out_weight = scatter_about(key_of[5], (HEADS * HEAD_DIM, D), (HEADS * HEAD_DIM) ** -0.5, 0.125, ((0, 8),))
    residual = scatter_about(key_of[6], (TOKENS, D), 1.0, 6.0, ((0, 32),))
    norm_gain = jnp.clip(1.0 + 0.18 * jax.random.normal(key_of[7], (D,), jnp.float32), 0.1, 1.9)
    gate_proj = scatter_about(key_of[8], (EXPERTS, D, FFE), D ** -0.5, 0.125, ((0, 4), (2, 8)))
    up_proj = scatter_about(key_of[9], (EXPERTS, D, FFE), D ** -0.5, 0.125, ((0, 4), (2, 8)))
    down_proj = scatter_about(key_of[10], (EXPERTS, FFE, D), FFE ** -0.5, 0.0625, ((0, 4), (1, 8)))
    expert_choice_keys = jax.random.split(jax.random.fold_in(key_of[11], 1), TOKENS // ROWS_DEV)
    expert_choice_turns = jax.random.permutation(jax.random.fold_in(key_of[11], 3), TOKENS // ROWS_DEV)
    expert_choice = jax.vmap(lambda own, number: assign_block(jax.random.fold_in(key_of[11], 2), own, number, ROWS_DEV, EXPERTS, 2, CAP, 1))(expert_choice_keys, expert_choice_turns).reshape((TOKENS, 2))
    expert_weights = jnp.clip(0.2 + 0.8 * jax.random.uniform(key_of[12], (TOKENS, 2), jnp.float32) ** block_levels(key_of[12], (TOKENS, 2), ((0, 32),), -0.2, 0.2), 0.2, 1.0)
    return {"queries": queries, "keys": keys, "values": values, "key_bias": key_bias, "head_gain": head_gain, "out_weight": out_weight, "residual": residual, "norm_gain": norm_gain, "gate_proj": gate_proj, "up_proj": up_proj, "down_proj": down_proj, "expert_choice": expert_choice, "expert_weights": expert_weights}


epsilon = 1e-06

def rms_scaled(values_in):
    return values_in * lax.rsqrt(lax.optimization_barrier(jnp.mean(values_in * values_in, axis=-1, keepdims=True)) + epsilon)

def head_mixture(operands):
    query_head, key_head, value_head, bias_head = operands
    length = query_head.shape[0]
    blocks = length // TOK_DEV
    scores = jnp.dot(query_head, key_head.T, preferred_element_type=jnp.float32) * HEAD_DIM ** (-0.5)
    scores = scores + bias_head.astype(jnp.float32)[None, :]
    position = jnp.arange(length, dtype=jnp.int32)
    earlier = (position[None, :] < position[:, None]).reshape(length, blocks, TOK_DEV)
    scores = scores.reshape(length, blocks, TOK_DEV)
    log_drops = jnp.where(earlier, jax.nn.log_sigmoid(-scores), 0.0)
    suffix = lax.cumsum(log_drops, axis=2, reverse=True) - log_drops
    within = jnp.where(earlier, jnp.exp(jax.nn.log_sigmoid(scores) + suffix), 0.0).astype(jnp.bfloat16)
    value_blocks = value_head.reshape(blocks, TOK_DEV, HEAD_DIM).astype(jnp.float32)
    block_sums = jnp.einsum('tms,msd->tmd', within.astype(jnp.float32), value_blocks)
    totals = lax.optimization_barrier(jnp.sum(log_drops, axis=2))
    carried = lax.optimization_barrier(jnp.sum(totals, axis=1, keepdims=True)) - jnp.cumsum(totals, axis=1)
    return lax.optimization_barrier(jnp.sum(jnp.exp(carried)[:, :, None] * block_sums, axis=1))

def reference(queries, keys, values, key_bias, head_gain, out_weight, residual, norm_gain, gate_proj, up_proj, down_proj, expert_choice, expert_weights):

    def split_heads(array):
        return array.reshape(TOKENS, HEADS, HEAD_DIM).transpose(1, 0, 2)
    mixture = lax.map(head_mixture, (split_heads(queries), split_heads(keys), split_heads(values), key_bias.T))
    attended = (rms_scaled(mixture) * head_gain[:, None, :]).astype(jnp.bfloat16)
    attended = attended.transpose(1, 0, 2).reshape(TOKENS, HEADS * HEAD_DIM)
    projected = jnp.dot(attended, out_weight, preferred_element_type=jnp.float32)
    stream = (residual.astype(jnp.float32) + projected).astype(jnp.bfloat16)
    normed = (rms_scaled(stream.astype(jnp.float32)) * norm_gain).astype(jnp.bfloat16)
    device_blocks = TOKENS // ROWS_DEV
    flat_expert = expert_choice.reshape(-1).astype(jnp.int32)
    flat_token = jnp.arange(2 * TOKENS, dtype=jnp.int32) // 2
    onehot = (flat_expert[:, None] == jnp.arange(EXPERTS, dtype=jnp.int32)[None, :]).astype(jnp.int32)
    grouped = onehot.reshape(device_blocks, 2 * ROWS_DEV, EXPERTS)
    before = (jnp.cumsum(grouped, axis=1) - grouped).reshape(2 * TOKENS, EXPERTS)
    slot_rank = lax.optimization_barrier(jnp.sum(before * onehot, axis=1)).astype(jnp.int32)
    slot_index = (flat_token // ROWS_DEV * CAP + slot_rank).astype(jnp.int32)
    slot_table = jnp.full((EXPERTS, device_blocks * CAP), TOKENS, jnp.int32).at[flat_expert, slot_index].set(flat_token)
    padded = jnp.concatenate([normed, jnp.zeros((1, D), jnp.bfloat16)], axis=0)
    group_size = FFE // N_TP

    def one_expert(operands):
        rows_index, gate_matrix, up_matrix, down_matrix = operands
        row_block = padded[rows_index]
        gate_part = jnp.dot(row_block, gate_matrix, preferred_element_type=jnp.float32)
        up_part = jnp.dot(row_block, up_matrix, preferred_element_type=jnp.float32)
        hidden = (jax.nn.silu(gate_part) * up_part).astype(jnp.bfloat16)
        hidden_groups = hidden.reshape(row_block.shape[0], N_TP, group_size).transpose(1, 0, 2)
        down_groups = down_matrix.reshape(N_TP, group_size, D)

        def add_group(running, group_pair):
            rounded = jnp.dot(group_pair[0], group_pair[1], preferred_element_type=jnp.float32).astype(jnp.bfloat16)
            rounded = lax.optimization_barrier(rounded)
            return (running + rounded.astype(jnp.float32), None)
        running, unused = lax.scan(add_group, jnp.zeros((row_block.shape[0], D), jnp.float32), (hidden_groups, down_groups))
        return running.astype(jnp.bfloat16)
    expert_out = lax.map(one_expert, (slot_table, gate_proj, up_proj, down_proj))
    picked = expert_out[flat_expert, slot_index].astype(jnp.float32).reshape(TOKENS, 2, D)
    combined = lax.optimization_barrier(jnp.sum(expert_weights[:, :, None] * picked, axis=1))
    return (stream.astype(jnp.float32) + combined).astype(jnp.bfloat16)
```

```python
import functools

import jax
import jax.numpy as jnp
from jax import lax
from jax.experimental import pallas as pl
from jax.experimental.pallas import tpu as pltpu
from jax.sharding import PartitionSpec as P

epsilon = 1e-06


def rms_scaled(values_in):
    return values_in * lax.rsqrt(jnp.mean(values_in * values_in, axis=-1, keepdims=True) + epsilon)


def expert_partial(row_block, gate_matrix, up_matrix, down_matrix):
    gate_part = jnp.dot(row_block, gate_matrix, preferred_element_type=jnp.float32)
    up_part = jnp.dot(row_block, up_matrix, preferred_element_type=jnp.float32)
    hidden = (jax.nn.silu(gate_part) * up_part).astype(jnp.bfloat16)
    return jnp.dot(hidden, down_matrix, preferred_element_type=jnp.float32)


def choice_ranks(routes, experts_all):
    flat_routes = routes.reshape(routes.shape[:-2] + (-1,))
    onehot = (flat_routes[..., None] == jnp.arange(experts_all, dtype=jnp.int32)).astype(jnp.int32)
    before = jnp.cumsum(onehot, axis=-2) - onehot
    return jnp.sum(before * onehot, axis=-1).reshape(routes.shape)


def slot_tokens(slot_index, targets, missing):
    flat_slots = slot_index.reshape(-1)
    owners = jnp.arange(flat_slots.shape[0], dtype=jnp.int32) // 2
    matches = flat_slots[None, :] == jnp.arange(targets, dtype=jnp.int32)[:, None]
    owner_found = jnp.sum(jnp.where(matches, owners[None, :], 0), axis=1)
    return jnp.where(jnp.any(matches, axis=1), owner_found, missing)


def softplus_parts(scores):
    drops = -jnp.maximum(scores, 0.0) - jnp.log(1.0 + jnp.exp(-jnp.abs(scores)))
    return drops, scores + drops


def attend_block(query_ref, key_of, value_of, bias_of, mix_ref, carry_ref, head_size, diagonal):
    rows, width = query_ref.shape
    lanes = 128 if width % 128 == 0 else width
    per_group = lanes // head_size
    chunk = 128 if rows % 128 == 0 else rows
    later_row = lax.broadcasted_iota(jnp.int32, (rows, rows), 0)
    later_col = lax.broadcasted_iota(jnp.int32, (rows, rows), 1)
    suffix_of = jnp.where(later_row > later_col, 1.0, 0.0).astype(jnp.bfloat16)
    lane_head = lax.broadcasted_iota(jnp.int32, (1, lanes), 1) // head_size
    for group in range(width // lanes):
        cols = slice(group * lanes, (group + 1) * lanes)
        key_tile = key_of(cols)
        value_tile = value_of(cols)
        for inner in range(per_group):
            mine = lane_head == inner
            bias_row = bias_of(group * per_group + inner)
            for start in range(0, rows, chunk):
                span = slice(start, start + chunk)
                query = query_ref[span, cols] * jnp.asarray(head_size**-0.5, jnp.bfloat16)
                query = jnp.where(mine, query, jnp.zeros_like(query))
                scores = lax.dot_general(
                    query, key_tile, (((1,), (1,)), ((), ())), preferred_element_type=jnp.float32
                )
                scores = scores + bias_row
                drops, hits = softplus_parts(scores)
                if diagonal:
                    row_pos = start + lax.broadcasted_iota(jnp.int32, (chunk, rows), 0)
                    col_pos = lax.broadcasted_iota(jnp.int32, (chunk, rows), 1)
                    earlier = col_pos < row_pos
                    drops = jnp.where(earlier, drops, 0.0)
                high = drops.astype(jnp.bfloat16)
                low = (drops - high.astype(jnp.float32)).astype(jnp.bfloat16)
                suffix = jnp.dot(high, suffix_of, preferred_element_type=jnp.float32)
                suffix = suffix + jnp.dot(low, suffix_of, preferred_element_type=jnp.float32)
                within = jnp.exp(hits + suffix)
                if diagonal:
                    within = jnp.where(earlier, within, 0.0)
                part = jnp.dot(
                    within.astype(jnp.bfloat16), value_tile, preferred_element_type=jnp.float32
                )
                total = suffix[:, 0:1] + drops[:, 0:1]
                if diagonal:
                    mix_old = jnp.zeros((chunk, lanes), jnp.float32)
                    carry_old = mix_old
                    if inner > 0:
                        mix_old = mix_ref[span, cols]
                        carry_old = carry_ref[span, cols]
                    mix_ref[span, cols] = jnp.where(mine, part, mix_old)
                    carry_ref[span, cols] = jnp.where(mine, total, carry_old)
                else:
                    mix_old = mix_ref[span, cols]
                    carry_old = carry_ref[span, cols]
                    mix_ref[span, cols] = jnp.where(
                        mine, mix_old + jnp.exp(carry_old) * part, mix_old
                    )
                    carry_ref[span, cols] = jnp.where(mine, carry_old + total, carry_old)


def diagonal_kernel(head_size, query_ref, key_ref, value_ref, bias_ref, mix_ref, carry_ref):
    attend_block(
        query_ref,
        lambda cols: key_ref[:, cols],
        lambda cols: value_ref[:, cols],
        lambda head: bias_ref[head : head + 1, :],
        mix_ref,
        carry_ref,
        head_size,
        True,
    )


def earlier_kernel(
    head_size, query_ref, pack_ref, bias_ref, mix_in, carry_in, gain_ref, out_ref, mix_ref, carry_ref
):
    rows, width = query_ref.shape
    lanes = 128 if width % 128 == 0 else width
    mix_ref[...] = mix_in[...]
    carry_ref[...] = carry_in[...]
    own = lax.axis_index("sp")

    def visit(step, nothing):
        block = own - 1 - step
        attend_block(
            query_ref,
            lambda cols: pack_ref[block, :rows, cols],
            lambda cols: pack_ref[block, :rows, slice(width + cols.start, width + cols.stop)],
            lambda head: bias_ref[block, head : head + 1, :],
            mix_ref,
            carry_ref,
            head_size,
            False,
        )
        return nothing

    lax.fori_loop(0, own, visit, 0)
    lane_head = lax.broadcasted_iota(jnp.int32, (1, lanes), 1) // head_size
    for group in range(width // lanes):
        cols = slice(group * lanes, (group + 1) * lanes)
        mixture = mix_ref[:, cols]
        squares = mixture * mixture
        scaled = mixture
        for inner in range(lanes // head_size):
            mine = lane_head == inner
            mean = jnp.sum(jnp.where(mine, squares, 0.0), axis=1, keepdims=True) / head_size
            scaled = jnp.where(mine, mixture * lax.rsqrt(mean + epsilon), scaled)
        out_ref[:, cols] = (scaled * gain_ref[:, cols]).astype(jnp.bfloat16)


def attention(queries, keys, values, key_bias, head_gain):
    rows, width = queries.shape
    heads, head_size = head_gain.shape
    blocks = lax.axis_size("sp")
    bias_own = key_bias.T
    extra = -(-heads * rows // (2 * width))
    padded = -(-(rows + extra) // 8) * 8 - rows
    flat_bias = jnp.pad(bias_own.reshape(-1), (0, padded * 2 * width - heads * rows))
    packed = jnp.concatenate(
        [jnp.concatenate([keys, values], axis=1), flat_bias.reshape(padded, 2 * width)], axis=0
    )
    gathered = lax.all_gather(packed, "sp", axis=0)
    vmem = pl.BlockSpec(memory_space=pltpu.VMEM)
    state = jax.ShapeDtypeStruct((rows, width), jnp.float32)
    work = heads * rows * rows
    mix, carry = pl.pallas_call(
        functools.partial(diagonal_kernel, head_size),
        out_shape=[state, state],
        in_specs=[vmem] * 4,
        out_specs=[vmem] * 2,
        cost_estimate=pl.CostEstimate(flops=work * 2000, bytes_accessed=10**6, transcendentals=0),
    )(queries, keys, values, bias_own.astype(jnp.float32))
    bias_all = gathered[:, rows:].reshape(blocks, -1)[:, : heads * rows]
    bias_all = bias_all.reshape(blocks, heads, rows).astype(jnp.float32)
    return pl.pallas_call(
        functools.partial(earlier_kernel, head_size),
        out_shape=jax.ShapeDtypeStruct((rows, width), jnp.bfloat16),
        in_specs=[vmem] * 6,
        out_specs=vmem,
        scratch_shapes=[pltpu.VMEM((rows, width), jnp.float32)] * 2,
        cost_estimate=pl.CostEstimate(flops=work * 4000, bytes_accessed=10**6, transcendentals=0),
    )(queries, gathered, bias_all, mix, carry, head_gain.reshape(1, width))


class Places:
    def __init__(self):
        self.sp = lax.axis_index("sp")
        self.tp = lax.axis_index("tp")
        self.depth = lax.axis_size("tp") // 2
        self.z = self.tp // 2
        self.core = self.tp % 2
        self.col = self.sp % 2
        self.line = self.sp // 2
        self.across = self.line * 2 + 1 - self.col
        self.along = (1 - self.line) * 2 + self.col
        self.far = (1 - self.line) * 2 + 1 - self.col
        self.partner = (self.sp, self.z * 2 + 1 - self.core)
        self.x_next = (self.across, self.tp)
        self.y_next = (self.along, self.tp)

    def z_peer(self, step):
        return lax.rem(self.z + step, self.depth)

    def z_device(self, step):
        return (self.sp, self.z_peer(step) * 2 + self.core)

    def meet(self, wide):
        barrier = pltpu.get_barrier_semaphore()
        peers = [self.partner] + [self.z_device(step) for step in range(1, self.depth)]
        if wide:
            peers = peers + [self.x_next, self.y_next]
        for peer in peers:
            pl.semaphore_signal(
                barrier, inc=1, device_id=peer, device_id_type=pl.DeviceIdType.MESH
            )
        pl.semaphore_wait(barrier, len(peers))


def remote(source, target, send_sem, recv_sem, device):
    return pltpu.make_async_remote_copy(
        src_ref=source,
        dst_ref=target,
        send_sem=send_sem,
        recv_sem=recv_sem,
        device_id=device,
        device_id_type=pl.DeviceIdType.MESH,
    )


def gather_kernel(own_ref, out_ref, local_sem, send_sems, recv_sems):
    place = Places()
    depth = place.depth
    place.meet(True)
    sends = []

    def slot(seq, z, core):
        return out_ref.at[seq, z, core]

    def send(source, seq, z, device, count):
        copy = remote(
            source,
            slot(seq, z, place.core),
            send_sems.at[count],
            recv_sems.at[seq, z, place.core],
            device,
        )
        copy.start()
        sends.append(copy)

    def arrived(seq, z, core):
        remote(
            own_ref, slot(seq, z, core), send_sems.at[0], recv_sems.at[seq, z, core], place.partner
        ).wait_recv()

    local = pltpu.make_async_copy(own_ref, slot(place.sp, place.z, place.core), local_sem)
    local.start()
    order = [0, 1] + list(range(depth - 1, 1, -1))
    for step in order[1:]:
        send(own_ref, place.sp, place.z, place.z_device(step), len(sends))
    for step in order:
        z = place.z_peer(step)
        source = own_ref
        if step > 0:
            arrived(place.sp, z, place.core)
            source = slot(place.sp, z, place.core)
        send(source, place.sp, z, place.x_next, len(sends))
        send(source, place.sp, z, place.y_next, len(sends))
        send(source, place.sp, z, place.partner, len(sends))
    for index, step in enumerate(order):
        z = place.z_peer(step)
        arrived(place.across, z, place.core)
        source = slot(place.across, z, place.core)
        if index % 2 == 0:
            send(source, place.across, z, place.y_next, len(sends))
        send(source, place.across, z, place.partner, len(sends))
        arrived(place.along, z, place.core)
        source = slot(place.along, z, place.core)
        if index % 2 == 1:
            send(source, place.along, z, place.x_next, len(sends))
        send(source, place.along, z, place.partner, len(sends))
    for step in order:
        z = place.z_peer(step)
        arrived(place.far, z, place.core)
        send(slot(place.far, z, place.core), place.far, z, place.partner, len(sends))
    for seq in (place.sp, place.across, place.along, place.far):
        for step in order:
            arrived(seq, place.z_peer(step), 1 - place.core)
    local.wait()
    for copy in sends:
        copy.wait_send()


def gather_rows(rows_in):
    rows, width = rows_in.shape
    depth = lax.axis_size("tp") // 2
    vmem = pl.BlockSpec(memory_space=pltpu.VMEM)
    count = depth - 1 + 3 * depth + 3 * depth + depth
    out = pl.pallas_call(
        gather_kernel,
        out_shape=jax.ShapeDtypeStruct((4, depth, 2, rows, width), rows_in.dtype),
        in_specs=[vmem],
        out_specs=vmem,
        scratch_shapes=[
            pltpu.SemaphoreType.DMA,
            pltpu.SemaphoreType.DMA((count,)),
            pltpu.SemaphoreType.DMA((4, depth, 2)),
        ],
        compiler_params=pltpu.CompilerParams(collective_id=1, has_side_effects=True),
    )(rows_in)
    return out.reshape(4 * depth * 2 * rows, width)


def add_into(target, first, *others):
    def one(z, nothing):
        total = first[z].astype(jnp.float32)
        for other in others:
            total = total + other[z].astype(jnp.float32)
        target[z] = total.astype(target.dtype)
        return nothing

    lax.fori_loop(0, target.shape[0], one, 0)


def finish_over_z(place, mine, z_recv, send_sems, recv_sems, base_ref, out_ref):
    copies = []
    order = [1] + list(range(place.depth - 1, 1, -1))
    for step in order:
        copy = remote(
            mine.at[place.z_peer(step)],
            z_recv.at[step - 1],
            send_sems.at[step - 1],
            recv_sems.at[step - 1],
            place.z_device(step),
        )
        copy.start()
        copies.append(copy)
    total = mine[place.z].astype(jnp.float32)
    for step, copy in zip(order, copies):
        copy.wait_recv()
        total = total + z_recv[step - 1].astype(jnp.float32)
    out_ref[...] = (base_ref[...].astype(jnp.float32) + total).astype(out_ref.dtype)
    for copy in copies:
        copy.wait_send()


def narrow_kernel(
    parts_ref, base_ref, out_ref, pair_recv, mine, z_recv, pair_send, pair_got, z_send, z_got
):
    place = Places()
    place.meet(False)
    copy = remote(
        parts_ref.at[1 - place.core], pair_recv, pair_send.at[0], pair_got.at[0], place.partner
    )
    copy.start()
    copy.wait_recv()
    add_into(mine, parts_ref.at[place.core], pair_recv)
    finish_over_z(place, mine, z_recv, z_send, z_got, base_ref, out_ref)
    copy.wait_send()


def wide_kernel(
    parts_ref,
    base_ref,
    out_ref,
    pair_recv,
    half_sum,
    x_recv,
    y_recv,
    x_last,
    y_last,
    mine,
    z_recv,
    pair_send,
    pair_got,
    xy_send,
    xy_got,
    z_send,
    z_got,
):
    place = Places()
    half = place.depth // 2
    front, back = pl.ds(0, half), pl.ds(half, place.depth - half)
    place.meet(True)
    order = (place.far, place.across, place.along, place.sp)
    pairs = []
    for count, seq in enumerate(order):
        copy = remote(
            parts_ref.at[1 - place.core, seq],
            pair_recv.at[count],
            pair_send.at[count],
            pair_got.at[count],
            place.partner,
        )
        copy.start()
        pairs.append(copy)
    sends = []

    def send(source, target, count, device):
        copy = remote(source, target, xy_send.at[count], xy_got.at[count], device)
        copy.start()
        sends.append(copy)
        return copy

    def pair_sum(count):
        pairs[count].wait_recv()
        add_into(half_sum.at[count], parts_ref.at[place.core, order[count]], pair_recv.at[count])

    pair_sum(0)
    far_x = send(half_sum.at[0, front], x_recv.at[1], 0, place.x_next)
    far_y = send(half_sum.at[0, back], y_recv.at[1], 1, place.y_next)
    pair_sum(1)
    near_x = send(half_sum.at[1, front], x_recv.at[0], 2, place.x_next)
    pair_sum(2)
    near_y = send(half_sum.at[2, back], y_recv.at[0], 3, place.y_next)
    pair_sum(3)
    far_x.wait_recv()
    add_into(x_recv.at[1], half_sum.at[2, front], x_recv.at[1])
    last_y = send(x_recv.at[1], y_last, 4, place.y_next)
    far_y.wait_recv()
    add_into(y_recv.at[1], half_sum.at[1, back], y_recv.at[1])
    last_x = send(y_recv.at[1], x_last, 5, place.x_next)
    near_x.wait_recv()
    near_y.wait_recv()
    last_y.wait_recv()
    add_into(mine.at[front], half_sum.at[3, front], x_recv.at[0], y_last)
    last_x.wait_recv()
    add_into(mine.at[back], half_sum.at[3, back], y_recv.at[0], x_last)
    finish_over_z(place, mine, z_recv, z_send, z_got, base_ref, out_ref)
    for copy in pairs + sends:
        copy.wait_send()


def scatter_sum(parts, base, out_dtype):
    rows, width = base.shape
    depth = lax.axis_size("tp") // 2
    vmem = pl.BlockSpec(memory_space=pltpu.VMEM)
    wide = parts.shape[0] > depth * 2 * rows
    half = depth // 2

    def room(*lead):
        return pltpu.VMEM(lead + (rows, width), jnp.bfloat16)

    def sems(count):
        return pltpu.SemaphoreType.DMA((count,))

    ends = [room(depth), room(depth - 1)]
    tail = [sems(depth - 1), sems(depth - 1)]
    if wide:
        shaped = parts.reshape(4, depth, 2, rows, width).transpose(2, 0, 1, 3, 4)
        body = wide_kernel
        scratch = [room(4, depth), room(4, depth), room(2, half), room(2, depth - half)]
        scratch = scratch + [room(depth - half), room(half)] + ends
        scratch = scratch + [sems(4), sems(4), sems(6), sems(6)] + tail
    else:
        shaped = parts.reshape(depth, 2, rows, width).transpose(1, 0, 2, 3)
        body = narrow_kernel
        scratch = [room(depth)] + ends + [sems(1), sems(1)] + tail
    return pl.pallas_call(
        body,
        out_shape=jax.ShapeDtypeStruct((rows, width), out_dtype),
        in_specs=[vmem] * 2,
        out_specs=vmem,
        scratch_shapes=scratch,
        compiler_params=pltpu.CompilerParams(
            collective_id=2 if wide else 0, has_side_effects=True, vmem_limit_bytes=60 * 2**20
        ),
    )(shaped, base)


def on_device(
    queries,
    keys,
    values,
    key_bias,
    head_gain,
    out_weight,
    residual,
    norm_gain,
    gate_proj,
    up_proj,
    down_proj,
    expert_choice,
    expert_weights,
):
    rows_own = queries.shape[0]
    model_width = out_weight.shape[1]
    seq_devices = lax.axis_size("sp")
    head_devices = lax.axis_size("tp")
    row_share = rows_own // head_devices
    local_experts = gate_proj.shape[0]
    experts_all = local_experts * seq_devices
    capacity = 4 * rows_own // (head_devices * experts_all)
    dense = capacity >= row_share and seq_devices == 4 and head_devices % 4 == 0
    if dense:
        named = expert_choice[:, :, None] == jnp.arange(experts_all, dtype=jnp.int32)
        own_weights = jnp.sum(jnp.where(named, expert_weights[:, :, None], 0.0), axis=1)
        all_weights = lax.all_gather(own_weights, ("sp", "tp"), axis=0, tiled=True)
        queries, all_weights = lax.optimization_barrier((queries, all_weights))
    attended = attention(queries, keys, values, key_bias, head_gain)
    shares = jnp.dot(attended, out_weight, preferred_element_type=jnp.float32)
    stream = scatter_sum(shares.astype(jnp.bfloat16), residual, jnp.bfloat16)
    normed = (rms_scaled(stream.astype(jnp.float32)) * norm_gain).astype(jnp.bfloat16)
    if dense:
        all_rows = gather_rows(normed)
        total = 0.0
        for local in range(local_experts):
            expert = lax.axis_index("sp") * local_experts + local
            weight = lax.dynamic_slice_in_dim(all_weights, expert, 1, 1)
            share = expert_partial(all_rows, gate_proj[local], up_proj[local], down_proj[local])
            total = total + jnp.where(weight > 0.0, weight * share, 0.0)
        return scatter_sum(total.astype(jnp.bfloat16), stream, jnp.bfloat16)
    own_slots = expert_choice * capacity + choice_ranks(expert_choice, experts_all)
    wanted = slot_tokens(own_slots, experts_all * capacity, row_share)
    outgoing = jnp.take(normed, wanted, axis=0, mode="fill", fill_value=0)
    arrived = lax.all_to_all(
        outgoing.reshape(seq_devices, local_experts, capacity, model_width),
        "sp",
        split_axis=0,
        concat_axis=0,
        tiled=True,
    )
    row_piece = lax.all_gather(arrived, "tp", axis=0, tiled=True)
    count_rows = row_piece.shape[0]
    partials = jnp.stack(
        [
            expert_partial(
                row_piece[:, 0].reshape(-1, model_width), gate_proj[0], up_proj[0], down_proj[0]
            ).reshape(count_rows, capacity, model_width)
        ],
        axis=1,
    )
    summed = lax.psum_scatter(partials.astype(jnp.bfloat16), "tp", scatter_dimension=0, tiled=True)
    returned = lax.all_to_all(summed, "sp", split_axis=0, concat_axis=0, tiled=True).reshape(
        experts_all * capacity, model_width
    )
    picked = jnp.take(returned, own_slots, axis=0).astype(jnp.float32)
    combined = jnp.sum(expert_weights[:, :, None] * picked, axis=1)
    return (stream.astype(jnp.float32) + combined).astype(jnp.bfloat16)


def solution(mesh):
    placed = (
        P("sp", "tp"),
        P("sp", "tp"),
        P("sp", "tp"),
        P("sp", "tp"),
        P("tp", None),
        P("tp", None),
        P(("sp", "tp"), None),
        P(),
        P("sp", None, "tp"),
        P("sp", None, "tp"),
        P("sp", "tp", None),
        P(("sp", "tp"), None),
        P(("sp", "tp"), None),
    )
    return jax.shard_map(
        on_device, mesh=mesh, in_specs=placed, out_specs=P(("sp", "tp"), None), check_vma=False
    )
```
